32 devices in a mesh: sp: 16 (over z, y, x), tp: 2 (over core).
Axes of the slice: x: 2, y: 2, z: 4, core: 2. Of those that a mesh axis runs over, the one named last changes fastest.
Arguments:
- residual: bfloat16 [2048, 2048], P('sp'), may hold values from -6 to 6
- query_nope: bfloat16 [2048, 8, 128], P('sp', 'tp'), may hold values from -6 to 6
- query_rope: bfloat16 [2048, 8, 64], P('sp', 'tp'), may hold values from -64 to 64
- latent: bfloat16 [2048, 256], P('sp'), may hold values from -6 to 6
- rope_key: bfloat16 [2048, 64], P('sp'), may hold values from -64 to 64
- kv_gain: bfloat16 [256], replicated, may hold values from 0.099609375 to 1.8984375
- key_up: bfloat16 [256, 8, 128], replicated, may hold values from -0.375 to 0.375
- value_up: bfloat16 [256, 8, 128], replicated, may hold values from -0.375 to 0.375
- out_weight: bfloat16 [1024, 2048], P('tp'), may hold values from -0.1875 to 0.1875
- post_gain: bfloat16 [2048], replicated, may hold values from 0.099609375 to 1.8984375
- pre_gain: bfloat16 [2048], replicated, may hold values from 0.099609375 to 1.8984375
- ffn_gain: bfloat16 [2048], replicated, may hold values from 0.099609375 to 1.8984375
- up_value: bfloat16 [2048, 5632], P('sp', 'tp'), may hold values from -0.125 to 0.125
- up_gate: bfloat16 [2048, 5632], P('sp', 'tp'), may hold values from -0.125 to 0.125
- conv_value: bfloat16 [3, 5632], replicated, may hold values from -3.5 to 3.5
- conv_gate: bfloat16 [3, 5632], replicated, may hold values from -3.5 to 3.5
- down_weight: bfloat16 [5632, 2048], P('tp', 'sp'), may hold values from -0.078125 to 0.078125
Outputs:
- layer_out: bfloat16 [2048, 2048], P(('sp', 'tp'))
The draws below stay inside these ranges and needn't reach their ends.
All inputs are finite; a program needn't handle non-finite values.
Results may differ from the reference program's by a relative error of at most 0.02.
Values may be sent and summed in bfloat16 or wider, within the bound.
A program may use at most 128 MiB of HBM per device.

```python
import jax
import jax.numpy as jnp
from jax import lax

D = 2048
HEADS = 8
NOPE = 128
ROPE = 64
VD = 128
KV = 256
FF = 5632
GRID = 64
TOKENS = 2048
N_TP = 2


def drawn_pair(key):
    folded = jax.random.fold_in(key, 41)
    query_key, rope_seed = jax.random.split(folded, 2)
    queries = jax.random.normal(query_key, (TOKENS, HEADS, ROPE), jnp.float32)
    rope_keys = jax.random.normal(rope_seed, (TOKENS, ROPE), jnp.float32)
    return (jnp.clip(queries, -64.0, 64.0), jnp.clip(rope_keys, -64.0, 64.0))


def draw_query_rope(key, part):
    return drawn_pair(key)[0].astype(jnp.bfloat16)


def draw_rope_key(key, part):
    return drawn_pair(key)[1].astype(jnp.bfloat16)


def level_of(key, shape, cuts, smallest, top_value):
    loudness = 1.0
    for dim, parts in cuts:
        draws = jax.random.uniform(jax.random.fold_in(jax.random.fold_in(key, 6), dim), (parts,), jnp.float32, smallest / len(cuts), top_value / len(cuts))
        loudness = loudness * jnp.repeat(jnp.exp(draws), shape[dim] // parts).reshape((-1,) + (1,) * (len(shape) - 1 - dim))
    return loudness


def bell_draw(rng, dims, scale, most, cuts=(), held_as=jnp.bfloat16):
    entries = scale * jax.random.normal(rng, dims, jnp.float32)
    if cuts:
        entries = entries * level_of(rng, dims, cuts, -0.22, 0.18)
    return jnp.clip(entries, -most, most).astype(held_as)


def setup_inputs(seed: int = 0) -> dict:
    arg_keys = jax.random.split(jax.random.key(seed), 18)
    return {
        "residual": bell_draw(arg_keys[0], (TOKENS, D), 1.0, 6.0, ((0, 16),)),
        "query_nope": bell_draw(arg_keys[1], (TOKENS, HEADS, NOPE), 1.0, 6.0, ((0, 16), (1, 2))),
        "query_rope": draw_query_rope(jax.random.fold_in(arg_keys[17], 71), 0),
        "latent": bell_draw(arg_keys[3], (TOKENS, KV), 1.0, 6.0, ((0, 16),)),
        "rope_key": draw_rope_key(jax.random.fold_in(arg_keys[17], 71), 0),
        "kv_gain": jnp.clip(1.0 + 0.18 * jax.random.normal(arg_keys[5], (KV,), jnp.float32), 0.099609375, 1.8984375).astype(jnp.bfloat16),
        "key_up": bell_draw(arg_keys[6], (KV, HEADS, NOPE), KV ** -0.5, 0.375),
        "value_up": bell_draw(arg_keys[7], (KV, HEADS, VD), KV ** -0.5, 0.375),
        "out_weight": bell_draw(arg_keys[8], (HEADS * VD, D), (HEADS * VD) ** -0.5, 0.1875, ((0, 2),)),
        "post_gain": jnp.clip(1.0 + 0.18 * jax.random.normal(arg_keys[9], (D,), jnp.float32), 0.099609375, 1.8984375).astype(jnp.bfloat16),
        "pre_gain": jnp.clip(1.0 + 0.18 * jax.random.normal(arg_keys[10], (D,), jnp.float32), 0.099609375, 1.8984375).astype(jnp.bfloat16),
        "ffn_gain": jnp.clip(1.0 + 0.18 * jax.random.normal(arg_keys[11], (D,), jnp.float32), 0.099609375, 1.8984375).astype(jnp.bfloat16),
        "up_value": bell_draw(arg_keys[12], (D, FF), D ** -0.5, 0.125, ((0, 16), (1, 2))),
        "up_gate": bell_draw(arg_keys[13], (D, FF), D ** -0.5, 0.125, ((0, 16), (1, 2))),
        "conv_value": bell_draw(arg_keys[14], (3, FF), 3 ** -0.5, 3.5),
        "conv_gate": bell_draw(arg_keys[15], (3, FF), 3 ** -0.5, 3.5),
        "down_weight": bell_draw(arg_keys[16], (FF, D), FF ** -0.5, 0.078125, ((0, 2), (1, 16))),
    }


epsilon = 1e-06
rope_base = 10000.0

def rms_norm(values, gain):
    return values * lax.rsqrt(lax.optimization_barrier(jnp.mean(values * values, axis=-1, keepdims=True)) + epsilon) * gain.astype(jnp.float32)

def widened(values):
    return lax.optimization_barrier(values.astype(jnp.bfloat16)).astype(jnp.float32)

def rotate(values, positions):
    pair_count = values.shape[-1] // 4
    frequency = rope_base ** (-jnp.arange(pair_count, dtype=jnp.float32) / pair_count)
    grid_rows = (positions // GRID).astype(jnp.float32)
    grid_cols = (positions % GRID).astype(jnp.float32)
    angles = jnp.stack([grid_rows, grid_cols], axis=-1)[:, :, None] * frequency
    table_shape = (angles.shape[0],) + (1,) * (values.ndim - 2) + angles.shape[1:]
    cosine = jnp.cos(angles).reshape(table_shape)
    sine = jnp.sin(angles).reshape(table_shape)
    halves = values.reshape(values.shape[:-1] + (2, 2, pair_count))
    leading = halves[..., 0, :]
    trailing = halves[..., 1, :]
    turned = jnp.stack([leading * cosine - trailing * sine, trailing * cosine + leading * sine], axis=-2)
    return turned.reshape(values.shape)

def reference(residual, query_nope, query_rope, latent, rope_key, kv_gain, key_up, value_up, out_weight, post_gain, pre_gain, ffn_gain, up_value, up_gate, conv_value, conv_gate, down_weight):
    token_count = residual.shape[0]
    positions = jnp.arange(token_count, dtype=jnp.int32)
    score_scale = (NOPE + ROPE) ** (-0.5)
    normed_wide = widened(rms_norm(latent.astype(jnp.float32), kv_gain))
    keys_nope = widened(jnp.einsum('nc,chd->nhd', normed_wide, key_up.astype(jnp.float32)))
    values_all = widened(jnp.einsum('nc,chd->nhd', normed_wide, value_up.astype(jnp.float32)))
    key_turn = widened(rotate(rope_key.astype(jnp.float32), positions))
    query_turn = widened(rotate(query_rope.astype(jnp.float32), positions))
    keys_all = jnp.concatenate([keys_nope, jnp.broadcast_to(key_turn[:, None, :], (token_count, HEADS, ROPE))], axis=-1)
    queries = jnp.concatenate([query_nope.astype(jnp.float32), query_turn], axis=-1)
    block_size = min(512, token_count)
    query_blocks = queries.reshape(token_count // block_size, block_size, HEADS, NOPE + ROPE)

    def attend_block(query_block):
        scores = jnp.einsum('qhd,khd->hqk', query_block, keys_all) * score_scale
        row_max = lax.optimization_barrier(jnp.max(scores, axis=-1, keepdims=True))
        weights = jnp.exp(scores - row_max)
        totals = lax.optimization_barrier(jnp.sum(weights, axis=-1))
        mixed = jnp.einsum('hqk,khd->qhd', widened(weights), values_all)
        return (mixed / jnp.transpose(totals)[:, :, None]).astype(jnp.bfloat16)
    attended = lax.map(attend_block, query_blocks).reshape(token_count, HEADS * VD)
    group_width = HEADS * VD // N_TP

    def add_heads(running, group_id):
        block_rows = lax.dynamic_slice_in_dim(attended, group_id * group_width, group_width, 1)
        weight_rows = lax.dynamic_slice_in_dim(out_weight, group_id * group_width, group_width, 0)
        partial_value = jnp.dot(block_rows, weight_rows, preferred_element_type=jnp.float32)
        return (running + widened(partial_value), None)
    summed = lax.scan(add_heads, jnp.zeros((token_count, D), jnp.float32), jnp.arange(N_TP, dtype=jnp.int32))[0]
    stream_wide = widened(residual.astype(jnp.float32) + rms_norm(widened(summed), post_gain))
    inputs = rms_norm(stream_wide, pre_gain).astype(jnp.bfloat16)
    value_rows = widened(jnp.dot(inputs, up_value, preferred_element_type=jnp.float32))
    gate_rows = widened(jnp.dot(inputs, up_gate, preferred_element_type=jnp.float32))

    def convolve(rows_wide, conv_taps):
        padded = jnp.pad(rows_wide, ((1, 1), (0, 0)))
        return padded[:-2] * conv_taps[0] + padded[1:-1] * conv_taps[1] + padded[2:] * conv_taps[2]
    value_conv = convolve(value_rows, conv_value.astype(jnp.float32))
    gate_conv = convolve(gate_rows, conv_gate.astype(jnp.float32))
    hidden = (jax.nn.silu(gate_conv) * value_conv).astype(jnp.bfloat16)
    ff_width = FF // N_TP

    def add_units(running, group_id):
        block_rows = lax.dynamic_slice_in_dim(hidden, group_id * ff_width, ff_width, 1)
        weight_rows = lax.dynamic_slice_in_dim(down_weight, group_id * ff_width, ff_width, 0)
        partial_value = jnp.dot(block_rows, weight_rows, preferred_element_type=jnp.float32)
        return (running + widened(partial_value), None)
    projected = lax.scan(add_units, jnp.zeros((token_count, D), jnp.float32), jnp.arange(N_TP, dtype=jnp.int32))[0]
    return (stream_wide + rms_norm(widened(projected), ffn_gain)).astype(jnp.bfloat16)
```

```python
import functools

import jax
import jax.numpy as jnp
from jax import lax
from jax.experimental import pallas as pl
from jax.experimental.pallas import tpu as pltpu
from jax.sharding import PartitionSpec as P

GRID = 64


epsilon = 1e-06
rope_base = 10000.0


def extended(x, sides, width):
    for axis, dim in sides:
        size, length = (lax.axis_size(axis), x.shape[dim])
        up = [(i, (i + 1) % size) for i in range(size - 1)]
        down = [(j, i) for i, j in up]
        last = lax.slice_in_dim(x, length - width, length, axis=dim)
        initial = lax.slice_in_dim(x, 0, width, axis=dim)
        before = lax.ppermute(last, axis, up)
        after = lax.ppermute(initial, axis, down)
        x = jnp.concatenate([before, x, after], axis=dim)
    return x


def rms_norm(values, gain):
    return (
        values
        * lax.rsqrt(jnp.mean(values * values, axis=-1, keepdims=True) + epsilon)
        * gain.astype(jnp.float32)
    )


def widened(values):
    return lax.optimization_barrier(values.astype(jnp.bfloat16)).astype(jnp.float32)


def rotate(values, positions):
    pair_count = values.shape[-1] // 4
    frequency = rope_base ** (-jnp.arange(pair_count, dtype=jnp.float32) / pair_count)
    grid_rows = (positions // GRID).astype(jnp.float32)
    grid_cols = (positions % GRID).astype(jnp.float32)
    angles = jnp.stack([grid_rows, grid_cols], axis=-1)[:, :, None] * frequency
    table_shape = (angles.shape[0],) + (1,) * (values.ndim - 2) + angles.shape[1:]
    cosine = jnp.cos(angles).reshape(table_shape)
    sine = jnp.sin(angles).reshape(table_shape)
    halves = values.reshape(values.shape[:-1] + (2, 2, pair_count))
    leading = halves[..., 0, :]
    trailing = halves[..., 1, :]
    turned = jnp.stack(
        [leading * cosine - trailing * sine, trailing * cosine + leading * sine], axis=-2
    )
    return turned.reshape(values.shape)


LANES = 128
CHUNKS = 2
MESH = pl.DeviceIdType.MESH


def kernel_fits(residual, latent, up_value):
    size = lax.axis_size("sp")
    return (
        size % 4 == 0
        and size >= 8
        and lax.axis_size("tp") == 2
        and residual.shape[0] == LANES
        and latent.shape[1] % LANES == 0
        and residual.shape[1] == size * LANES
        and up_value.shape[1] % LANES == 0
        and up_value.shape[1] // LANES >= size // 2
    )


def turned_rows(values, first_position):
    quarter = values.shape[0] // 4
    pair = lax.broadcasted_iota(jnp.int32, (quarter, values.shape[1]), 0).astype(jnp.float32)
    frequency = jnp.exp(pair * (-jnp.log(jnp.float32(rope_base)) / quarter))
    positions = first_position + lax.broadcasted_iota(jnp.int32, (quarter, values.shape[1]), 1)
    shift = GRID.bit_length() - 1
    places = (jnp.right_shift(positions, shift), jnp.bitwise_and(positions, GRID - 1))
    out = []
    for half, place in enumerate(places):
        angles = place.astype(jnp.float32) * frequency
        cosine, sine = jnp.cos(angles), jnp.sin(angles)
        a = values[2 * half * quarter : (2 * half + 1) * quarter]
        b = values[(2 * half + 1) * quarter : (2 * half + 2) * quarter]
        out += [a * cosine - b * sine, b * cosine + a * sine]
    return jnp.concatenate(out, axis=0)


def layer_kernel(
    sizes,
    residual,
    q_abs,
    q_rope,
    latent,
    rope_key,
    kv_gain,
    value_local,
    out_weight,
    gains,
    taps,
    up_value,
    up_gate,
    down,
    out,
    lat,
    queries,
    keys_t,
    attended,
    out_w,
    res,
    wup,
    wdn,
    head_part,
    head_came,
    stream,
    xs,
    ups,
    edges,
    edges_came,
    parts,
    core_came,
    y_sums,
    y_came,
    z_sums,
    z_came,
    l_recv,
    l_send_z,
    l_send_y,
    l_send_x,
    l_send_c,
    w_recv,
    w_send,
    wf_send,
    w_loc,
    t_sem,
    x_recv,
    x_up,
    x_dn,
    x_y,
    x_c,
    e_send,
    e_recv,
    c_send,
    c_recv,
    y_send,
    y_recv,
    z_send,
    z_recv,
    ld,
):
    n_sp, tile_count, tiles_max, ff_dev, score_scale = sizes
    nz, places = n_sp // 4, n_sp // 2
    tok, width = residual.shape
    half = tok // 2
    heads = q_abs.shape[0]
    kv = latent.shape[1]
    unit = tiles_max * LANES
    cw = width // CHUNKS
    me, c = lax.axis_index("sp"), lax.axis_index("tp")
    z, y, x = me // 4, me // 2 % 2, me % 2
    my_place = me // 2
    peer_c, peer_x, peer_y = (me, 1 - c), (me + 1 - 2 * x, c), (me + 2 - 4 * y, c)

    def dev(zz, yy):
        return (zz * 4 + yy * 2 + x, c)

    def remote(src, dst, send, recv, to):
        return pltpu.make_async_remote_copy(
            src_ref=src, dst_ref=dst, send_sem=send, recv_sem=recv, device_id=to, device_id_type=MESH
        )

    def z_order(i):
        below, above = z, nz - 1 - z
        both = jnp.minimum(below, above)
        paired = i <= 2 * both
        dist = jnp.where(paired, (i + 1) // 2, i - both)
        down_first = jnp.where(paired, i % 2 == 1, below > above)
        return jnp.where(i == 0, z, jnp.where(down_first, z - dist, z + dist))

    barrier = pltpu.get_barrier_semaphore()
    pl.semaphore_signal(barrier, inc=1, device_id=peer_c, device_id_type=MESH)
    pl.semaphore_signal(barrier, inc=1, device_id=peer_x, device_id_type=MESH)

    @pl.loop(1, places)
    def _(k):
        p = (my_place + k) % places
        pl.semaphore_signal(barrier, inc=1, device_id=(p * 2 + x, c), device_id_type=MESH)

    def local(src, dst, sem):
        return pltpu.make_async_copy(src, dst, sem)

    def tiles_of(p):
        first, last = p * tile_count // places, (p + 1) * tile_count // places
        return jnp.minimum(first, tile_count - tiles_max), first, last

    def offset_of(p):
        return pl.multiple_of(tiles_of(p)[0] * LANES, LANES)

    def up_rows(s):
        return pl.ds(pl.multiple_of(s * tok, tok), tok)

    own_units = pl.ds(offset_of(my_place), unit)
    own_copies = [
        local(up_value.at[:, own_units], wup.at[up_rows(me), pl.ds(0, unit)], w_loc.at[0]),
        local(up_gate.at[:, own_units], wup.at[up_rows(me), pl.ds(unit, unit)], w_loc.at[1]),
        local(down.at[own_units, :], wdn.at[:, up_rows(me)], w_loc.at[2]),
    ]
    loads = [
        local(out_weight, out_w, ld.at[0]),
        local(residual.at[pl.ds(pl.multiple_of(c * half, half), half), :], res, ld.at[1]),
    ]
    for copy in own_copies + loads:
        copy.start()

    def lat_rows(s, core):
        return lat.at[pl.ds(pl.multiple_of((s * 2 + core) * half, half), half), :]

    mine = pl.ds(pl.multiple_of(c * half, half), half)
    own = latent[mine, :].astype(jnp.float32)
    normed = (
        own * lax.rsqrt(jnp.mean(own * own, axis=-1, keepdims=True) + epsilon) * kv_gain[...]
    )
    keys_t[...] = turned_rows(rope_key[...].astype(jnp.float32), me * tok).T
    key_turn = keys_t[mine, :]
    own_lat = pl.ds(pl.multiple_of((me * 2 + c) * half, half), half)
    lat[own_lat, 0:kv] = normed.astype(jnp.bfloat16)
    lat[own_lat, kv : kv + LANES] = jnp.concatenate(
        [key_turn, jnp.zeros((half, LANES - key_turn.shape[1]), jnp.float32)], axis=1
    ).astype(jnp.bfloat16)

    pl.semaphore_wait(barrier, places + 1)

    def lat_copy(s, core, send, to):
        i = s * 2 + core
        return remote(lat_rows(s, core), lat_rows(s, core), send, l_recv.at[i], to)

    def lat_wait(s, core):
        lat_copy(s, core, l_send_z.at[0], peer_c).wait_recv()

    for d in range(1, nz):
        lat_copy(me, c, l_send_z.at[d - 1], dev((z + d) % nz, y)).start()
    lat_copy(me, c, l_send_y.at[0], peer_y).start()
    lat_copy(me, c, l_send_x.at[0], peer_x).start()
    lat_copy(me, c, l_send_c.at[0], peer_c).start()

    def weight_copies(p):
        units = pl.ds(offset_of(p), unit)
        to = (p * 2 + x, c)
        return [
            remote(up_value.at[:, units], wup.at[up_rows(me), pl.ds(0, unit)], w_send.at[p, 0], w_recv.at[me, 0], to),
            remote(up_gate.at[:, units], wup.at[up_rows(me), pl.ds(unit, unit)], w_send.at[p, 1], w_recv.at[me, 1], to),
            remote(down.at[units, :], wdn.at[:, up_rows(me)], w_send.at[p, 2], w_recv.at[me, 2], to),
        ]

    def arrivals(s):
        units = pl.ds(0, unit)
        return [
            remote(wup.at[up_rows(s), pl.ds(0, unit)], wup.at[up_rows(s), pl.ds(0, unit)], w_send.at[0, 0], w_recv.at[s, 0], peer_x),
            remote(wup.at[up_rows(s), pl.ds(unit, unit)], wup.at[up_rows(s), pl.ds(unit, unit)], w_send.at[0, 1], w_recv.at[s, 1], peer_x),
            remote(wdn.at[:, up_rows(s)], wdn.at[:, up_rows(s)], w_send.at[0, 2], w_recv.at[s, 2], peer_x),
        ]

    def forward_copies(p, s):
        return [
            remote(wup.at[up_rows(s), :], wup.at[up_rows(s), :], wf_send.at[p, 0], w_recv.at[s, 0], peer_x),
            remote(wdn.at[:, up_rows(s)], wdn.at[:, up_rows(s)], wf_send.at[p, 1], w_recv.at[s, 2], peer_x),
        ]

    def pass_on(zz, yy):
        p = zz * 2 + yy
        s = p * 2 + x
        for copy in arrivals(s):
            copy.wait_recv()
        for copy in forward_copies(p, s):
            copy.start()

    @pl.loop(1, nz)
    def _(d):
        for copy in weight_copies((z + d) % nz * 2 + y):
            copy.start()

    @pl.loop(1, nz)
    def _(d):
        s = (z + d) % nz * 4 + y * 2 + x
        lat_wait(s, c)
        lat_copy(s, c, l_send_y.at[d], peer_y).start()
        lat_copy(s, c, l_send_x.at[d], peer_x).start()
        lat_copy(s, c, l_send_c.at[d], peer_c).start()

    @pl.loop(0, nz)
    def _(d):
        s = (z + d) % nz * 4 + (1 - y) * 2 + x
        lat_wait(s, c)
        lat_copy(s, c, l_send_x.at[nz + d], peer_x).start()
        lat_copy(s, c, l_send_c.at[nz + d], peer_c).start()

    @pl.loop(0, nz)
    def _(d):
        for copy in weight_copies((z + d) % nz * 2 + 1 - y):
            copy.start()

    for h in range(heads):
        turned = turned_rows(q_rope[h].astype(jnp.float32), me * tok).T
        queries[h, :, 0:kv] = q_abs[h]
        queries[h, :, kv : kv + LANES] = jnp.concatenate(
            [turned, jnp.zeros((tok, LANES - turned.shape[1]), jnp.float32)], axis=1
        ).astype(jnp.bfloat16)

    @pl.loop(0, 2 * nz)
    def _(i):
        s = (z + i // 2) % nz * 4 + (y + i) % 2 * 2 + 1 - x
        lat_wait(s, c)
        lat_copy(s, c, l_send_c.at[2 * nz + i], peer_c).start()

    for copy in own_copies:
        copy.wait()
    for copy in forward_copies(my_place, me):
        copy.start()

    @pl.loop(0, n_sp)
    def _(s):
        lat_wait(s, 1 - c)

    @pl.loop(0, heads)
    def _(h):
        scores = lax.dot_general(
            queries[h], lat[...], (((1,), (1,)), ((), ())), preferred_element_type=jnp.float32
        )
        top = jnp.max(scores, axis=-1, keepdims=True)
        weights = jnp.exp((scores - top) * score_scale)
        totals = jnp.sum(weights, axis=-1, keepdims=True)
        mixed = jnp.dot(weights.astype(jnp.bfloat16), lat[:, 0:kv], preferred_element_type=jnp.float32)
        mixed = (mixed / totals).astype(jnp.bfloat16)
        columns = pl.ds(pl.multiple_of(h * value_local.shape[2], LANES), value_local.shape[2])
        attended[:, columns] = jnp.dot(
            mixed, value_local[h], preferred_element_type=jnp.float32
        ).astype(jnp.bfloat16)

    @pl.loop(1, nz)
    def _(i):
        pass_on(z_order(i), y)

    loads[0].wait()

    @pl.loop(0, width // 512)
    def _(n):
        columns = pl.ds(pl.multiple_of(n * 512, 512), 512)
        head_part[:, columns] = jnp.dot(
            attended[...], out_w[:, columns], preferred_element_type=jnp.float32
        ).astype(jnp.bfloat16)

    other = pl.ds(pl.multiple_of((1 - c) * half, half), half)
    swap = remote(head_part.at[other, :], head_came, t_sem.at[0], t_sem.at[1], peer_c)
    swap.start()
    loads[1].wait()
    swap.wait_recv()
    summed = head_part[mine, :].astype(jnp.float32) + head_came[...].astype(jnp.float32)
    summed = summed.astype(jnp.bfloat16).astype(jnp.float32)
    scaled = summed * lax.rsqrt(jnp.mean(summed * summed, axis=-1, keepdims=True) + epsilon)
    wide = (res[...].astype(jnp.float32) + scaled * gains[0:1, :]).astype(jnp.bfloat16)
    stream[...] = wide
    wide = wide.astype(jnp.float32)
    inputs = wide * lax.rsqrt(jnp.mean(wide * wide, axis=-1, keepdims=True) + epsilon)
    own_row = pl.ds(pl.multiple_of(my_place * tok + c * half, half), half)
    xs[own_row, :] = (inputs * gains[1:2, :]).astype(jnp.bfloat16)

    def x_part(b, core, q):
        return xs.at[pl.ds(pl.multiple_of(b * tok + core * half, half), half), pl.ds(pl.multiple_of(q * cw, cw), cw)]

    def x_copy(b, core, q, send, to):
        part = x_part(b, core, q)
        return remote(part, part, send.at[b, q], x_recv.at[b, core, q], to)

    def x_sends(bz, by, q, act):
        b = bz * 2 + by
        along = by == y

        @pl.when(along & (bz <= z) & (z < nz - 1))
        def _():
            act(x_copy(b, c, q, x_up, dev(jnp.minimum(z + 1, nz - 1), y)))

        @pl.when(along & (bz >= z) & (z > 0))
        def _():
            act(x_copy(b, c, q, x_dn, dev(jnp.maximum(z - 1, 0), y)))

        @pl.when(along)
        def _():
            act(x_copy(b, c, q, x_y, peer_y))

        act(x_copy(b, c, q, x_c, peer_c))

    def start(copy):
        copy.start()

    for q in range(CHUNKS):
        x_sends(z, y, q, start)

    def x_step(k, cross):
        bz = z_order(k)
        by = jnp.where(cross, 1 - y, y)
        for q in range(CHUNKS):
            x_copy(bz * 2 + by, c, q, x_c, peer_c).wait_recv()
            x_sends(bz, by, q, start)

    @pl.loop(0, nz)
    def _(i):
        @pl.when(i < nz - 1)
        def _():
            x_step(i + 1, False)

        x_step(i, True)
        pass_on(z_order(i), 1 - y)

    @pl.loop(0, places)
    def _(p):
        s = p * 2 + 1 - x
        for copy in forward_copies(p, s):
            copy.wait_recv()

    for b_q in range(CHUNKS):

        @pl.loop(0, places)
        def _(b):
            x_copy(b, 1 - c, b_q, x_c, peer_c).wait_recv()

    rows_step = 2 * tok

    @pl.loop(0, places * tok // rows_step)
    def _(i):
        rows = pl.ds(pl.multiple_of(i * rows_step, rows_step), rows_step)
        ups[rows, :] = jnp.dot(
            xs[rows, :], wup[...], preferred_element_type=jnp.float32
        ).astype(jnp.bfloat16)

    def edge_copy(b):
        return remote(edges.at[b], edges_came.at[b], e_send.at[b], e_recv.at[b], peer_x)

    @pl.loop(0, places)
    def _(b):
        first = ups[pl.ds(pl.multiple_of(b * tok, tok), 16), :].astype(jnp.float32)[0:1]
        last = ups[pl.ds(pl.multiple_of(b * tok + tok - 16, 16), 16), :].astype(jnp.float32)[15:16]
        row = lax.broadcasted_iota(jnp.int32, (8, 2 * unit), 0)
        edges[b] = jnp.where(row == 0, first, last)
        edge_copy(b).start()

    @pl.loop(0, places)
    def _(b):
        edge_copy(b).wait_recv()

    start_tile, first_tile, last_tile = tiles_of(my_place)
    tap_columns = pl.ds(pl.multiple_of(c * ff_dev + start_tile * LANES, LANES), unit)
    tap = taps[:, tap_columns]
    taps_wide = jnp.concatenate([tap[0:3], tap[3:6]], axis=1)
    column = lax.broadcasted_iota(jnp.int32, (1, unit), 1)
    kept = (column >= (first_tile - start_tile) * LANES) & (column < (last_tile - start_tile) * LANES)

    def part_of(b):
        rows = ups[pl.ds(pl.multiple_of(b * tok, tok), tok), :].astype(jnp.float32)
        before = edges_came[jnp.maximum(b - 1 + x, 0)][1:2]
        before = jnp.where(b - 1 + x >= 0, before, 0.0)
        after = edges_came[jnp.minimum(b + x, places - 1)][0:1]
        after = jnp.where(b + x <= places - 1, after, 0.0)
        row = lax.broadcasted_iota(jnp.int32, rows.shape, 0)
        previous = jnp.where(row == 0, before, pltpu.roll(rows, 1, 0))
        following = jnp.where(row == tok - 1, after, pltpu.roll(rows, tok - 1, 0))
        mixed = previous * taps_wide[0:1] + rows * taps_wide[1:2] + following * taps_wide[2:3]
        gate = mixed[:, unit:]
        hidden = gate / (1.0 + jnp.exp(-gate)) * mixed[:, :unit]
        hidden = jnp.where(kept, hidden, 0.0).astype(jnp.bfloat16)
        parts[pl.ds(pl.multiple_of(b * tok, tok), tok), :] = jnp.dot(
            hidden, wdn[...], preferred_element_type=jnp.float32
        ).astype(jnp.bfloat16)

    def part_rows(b, core):
        return pl.ds(pl.multiple_of(b * tok + core * half, half), half)

    def core_copy(b):
        return remote(parts.at[part_rows(b, 1 - c), :], core_came.at[b], c_send.at[b], c_recv.at[b], peer_c)

    def core_sum(b):
        core_copy(b).wait_recv()
        return parts[part_rows(b, c), :].astype(jnp.float32) + core_came[b].astype(jnp.float32)

    def y_copy(zz):
        return remote(y_sums.at[zz], y_came.at[zz], y_send.at[zz], y_recv.at[zz], peer_y)

    def z_copy(zz):
        return remote(z_sums.at[zz], z_came.at[z], z_send.at[zz], z_recv.at[z], dev(zz, y))

    def z_arrival(zz):
        return remote(z_sums.at[zz], z_came.at[zz], z_send.at[zz], z_recv.at[zz], dev(zz, y))

    @pl.loop(0, nz)
    def _(i):
        zz = (z + 1 + i) % nz
        part_of(zz * 2 + 1 - y)
        core_copy(zz * 2 + 1 - y).start()
        y_sums[zz] = core_sum(zz * 2 + 1 - y).astype(jnp.bfloat16)
        y_copy(zz).start()

    @pl.loop(0, nz)
    def _(i):
        zz = (z + 1 + i) % nz
        part_of(zz * 2 + y)
        core_copy(zz * 2 + y).start()

    @pl.loop(0, nz)
    def _(i):
        zz = (z + 1 + i) % nz
        total = core_sum(zz * 2 + y)
        y_copy(zz).wait_recv()
        z_sums[zz] = (total + y_came[zz].astype(jnp.float32)).astype(jnp.bfloat16)

        @pl.when(zz != z)
        def _():
            z_copy(zz).start()

    projected = z_sums[z].astype(jnp.float32)
    for d in range(1, nz):
        zz = (z + nz - d) % nz
        z_arrival(zz).wait_recv()
        projected = projected + z_came[zz].astype(jnp.float32)
    projected = projected.astype(jnp.bfloat16).astype(jnp.float32)
    scaled = projected * lax.rsqrt(jnp.mean(projected * projected, axis=-1, keepdims=True) + epsilon)
    out[...] = (stream[...].astype(jnp.float32) + scaled * gains[2:3, :]).astype(jnp.bfloat16)

    for d in range(1, nz):
        lat_copy(me, c, l_send_z.at[d - 1], peer_c).wait_send()

    @pl.loop(0, nz)
    def _(d):
        lat_copy(me, c, l_send_y.at[d], peer_c).wait_send()

    @pl.loop(0, 2 * nz)
    def _(d):
        lat_copy(me, c, l_send_x.at[d], peer_c).wait_send()

    @pl.loop(0, 4 * nz)
    def _(d):
        lat_copy(me, c, l_send_c.at[d], peer_c).wait_send()

    swap.wait_send()

    @pl.loop(0, places)
    def _(p):
        @pl.when(p != my_place)
        def _():
            for copy in weight_copies(p):
                copy.wait_send()

        for copy in forward_copies(p, p * 2 + x):
            copy.wait_send()
        for q in range(CHUNKS):
            x_sends(p // 2, p % 2, q, lambda copy: copy.wait_send())
        edge_copy(p).wait_send()
        core_copy(p).wait_send()

    @pl.loop(0, nz)
    def _(zz):
        y_copy(zz).wait_send()

        @pl.when(zz != z)
        def _():
            z_copy(zz).wait_send()


def fused_layer(
    residual,
    query_nope,
    query_rope,
    latent,
    rope_key,
    kv_gain,
    key_up,
    value_up,
    out_weight,
    post_gain,
    pre_gain,
    ffn_gain,
    up_value,
    up_gate,
    conv_value,
    conv_gate,
    down_weight,
):
    n_sp = lax.axis_size("sp")
    nz, places = n_sp // 4, n_sp // 2
    tok, width = residual.shape
    half = tok // 2
    heads, kv = query_nope.shape[1], latent.shape[1]
    rope = rope_key.shape[1]
    value_width = value_up.shape[2]
    ff_dev = up_value.shape[1]
    tile_count = ff_dev // LANES
    tiles_max = -(-tile_count // places)
    unit = tiles_max * LANES
    score_scale = (query_nope.shape[2] + rope) ** (-0.5)
    first_head = lax.axis_index("tp") * heads
    key_local = lax.dynamic_slice_in_dim(key_up, first_head, heads, 1)
    value_local = lax.dynamic_slice_in_dim(value_up, first_head, heads, 1)
    q_abs = jnp.einsum(
        "qhd,chd->hqc", query_nope, key_local, preferred_element_type=jnp.float32
    ).astype(jnp.bfloat16)
    value_local = jnp.transpose(value_local, (1, 0, 2))
    gains = jnp.stack([post_gain, pre_gain, ffn_gain]).astype(jnp.float32)
    taps = jnp.concatenate([conv_value, conv_gate], axis=0).astype(jnp.float32)
    dma, vmem = pltpu.SemaphoreType.DMA, pltpu.VMEM
    bf16, f32 = jnp.bfloat16, jnp.float32
    scratch = [
        vmem((n_sp * tok, kv + LANES), bf16),
        vmem((heads, tok, kv + LANES), bf16),
        vmem((tok, rope), f32),
        vmem((tok, heads * value_width), bf16),
        vmem(out_weight.shape, bf16),
        vmem((half, width), bf16),
        vmem((n_sp * tok, 2 * unit), bf16),
        vmem((unit, n_sp * tok), bf16),
        vmem((tok, width), bf16),
        vmem((half, width), bf16),
        vmem((half, width), bf16),
        vmem((places * tok, width), bf16),
        vmem((places * tok, 2 * unit), bf16),
        vmem((places, 8, 2 * unit), f32),
        vmem((places, 8, 2 * unit), f32),
        vmem((places * tok, width), bf16),
        vmem((places, half, width), bf16),
        vmem((nz, half, width), bf16),
        vmem((nz, half, width), bf16),
        vmem((nz, half, width), bf16),
        vmem((nz, half, width), bf16),
        dma((n_sp * 2,)),
        dma((nz,)),
        dma((nz,)),
        dma((2 * nz,)),
        dma((4 * nz,)),
        dma((n_sp, 3)),
        dma((places, 3)),
        dma((places, 2)),
        dma((3,)),
        dma((2,)),
        dma((places, 2, CHUNKS)),
        dma((places, CHUNKS)),
        dma((places, CHUNKS)),
        dma((places, CHUNKS)),
        dma((places, CHUNKS)),
        dma((places,)),
        dma((places,)),
        dma((places,)),
        dma((places,)),
        dma((nz,)),
        dma((nz,)),
        dma((nz,)),
        dma((nz,)),
        dma((2,)),
    ]
    whole, apart = pl.BlockSpec(memory_space=pltpu.VMEM), pl.BlockSpec(memory_space=pl.ANY)
    sizes = (n_sp, tile_count, tiles_max, ff_dev, score_scale)
    return pl.pallas_call(
        functools.partial(layer_kernel, sizes),
        out_shape=jax.ShapeDtypeStruct((half, width), bf16),
        in_specs=[apart] + [whole] * 6 + [apart] + [whole] * 2 + [apart] * 3,
        out_specs=whole,
        scratch_shapes=scratch,
        compiler_params=pltpu.CompilerParams(
            collective_id=0, has_side_effects=True, vmem_limit_bytes=60 * 1024 * 1024
        ),
    )(
        residual,
        q_abs,
        jnp.transpose(query_rope, (1, 2, 0)),
        latent,
        rope_key.T,
        kv_gain.astype(f32).reshape(1, kv),
        value_local,
        out_weight,
        gains,
        taps,
        up_value,
        up_gate,
        down_weight,
    )


def body(
    residual,
    query_nope,
    query_rope,
    latent,
    rope_key,
    kv_gain,
    key_up,
    value_up,
    out_weight,
    post_gain,
    pre_gain,
    ffn_gain,
    up_value,
    up_gate,
    conv_value,
    conv_gate,
    down_weight,
):
    if kernel_fits(residual, latent, up_value):
        return fused_layer(
            residual,
            query_nope,
            query_rope,
            latent,
            rope_key,
            kv_gain,
            key_up,
            value_up,
            out_weight,
            post_gain,
            pre_gain,
            ffn_gain,
            up_value,
            up_gate,
            conv_value,
            conv_gate,
            down_weight,
        )
    tok_rows = residual.shape[0]
    heads_dev = query_nope.shape[1]
    value_width = value_up.shape[2]
    tp_index = lax.axis_index("tp")
    positions = lax.axis_index("sp") * tok_rows + jnp.arange(tok_rows, dtype=jnp.int32)
    score_scale = (query_nope.shape[2] + query_rope.shape[2]) ** (-0.5)
    normed = rms_norm(latent.astype(jnp.float32), kv_gain).astype(jnp.bfloat16)
    key_turn = rotate(rope_key.astype(jnp.float32), positions).astype(jnp.bfloat16)
    query_turn = rotate(query_rope.astype(jnp.float32), positions).astype(jnp.bfloat16)
    key_local = lax.dynamic_slice_in_dim(key_up, tp_index * heads_dev, heads_dev, 1)
    value_local = lax.dynamic_slice_in_dim(value_up, tp_index * heads_dev, heads_dev, 1)
    latent_width = normed.shape[1]
    joined = jnp.concatenate([normed, key_turn], axis=1)
    joined = lax.all_gather(joined, "sp", axis=0, tiled=True)
    pieces = (joined[:, :latent_width], joined[:, latent_width:])
    keys_nope = jnp.einsum(
        "nc,chd->nhd", pieces[0], key_local, preferred_element_type=jnp.float32
    ).astype(jnp.bfloat16)
    values_part = jnp.einsum(
        "nc,chd->nhd", pieces[0], value_local, preferred_element_type=jnp.float32
    ).astype(jnp.bfloat16)
    row_max = jnp.full((heads_dev, tok_rows), -1e30, jnp.float32)
    scores = (
        jnp.einsum("qhd,khd->hqk", query_nope, keys_nope, preferred_element_type=jnp.float32)
        + jnp.einsum("qhd,kd->hqk", query_turn, pieces[1], preferred_element_type=jnp.float32)
    ) * score_scale
    new_max = jnp.maximum(row_max, jnp.max(scores, axis=-1))
    weights = jnp.exp(scores - new_max[:, :, None])
    totals = jnp.sum(weights, axis=-1)
    weighted = jnp.einsum(
        "hqk,khd->hqd",
        weights.astype(jnp.bfloat16),
        values_part,
        preferred_element_type=jnp.float32,
    )
    attended = (weighted / totals[:, :, None]).astype(jnp.bfloat16)
    attended = jnp.transpose(attended, (1, 0, 2)).reshape(tok_rows, heads_dev * value_width)
    row_share = tok_rows // lax.axis_size("tp")
    summed = lax.psum_scatter(
        jnp.dot(attended, out_weight, preferred_element_type=jnp.float32).astype(jnp.bfloat16),
        "tp",
        scatter_dimension=0,
        tiled=True,
    ).astype(jnp.float32)
    own_rows = lax.dynamic_slice_in_dim(residual, tp_index * row_share, row_share, 0).astype(
        jnp.float32
    )
    stream_wide = widened(own_rows + rms_norm(widened(summed), post_gain))
    own_inputs = rms_norm(stream_wide, pre_gain).astype(jnp.bfloat16)
    inputs = lax.all_gather(own_inputs, "tp", axis=0, tiled=True)
    ff_dev = up_value.shape[1]
    up_joined = jnp.concatenate([up_value, up_gate], axis=1)
    up_whole = lax.all_gather(up_joined, "sp", axis=0, tiled=True)
    up_pair = jnp.dot(inputs, up_whole, preferred_element_type=jnp.float32).astype(jnp.bfloat16)
    padded = extended(up_pair, (("sp", 0),), 1).astype(jnp.float32)
    channel_start = tp_index * ff_dev
    conv_taps = jnp.concatenate(
        [
            lax.dynamic_slice_in_dim(conv_value, channel_start, ff_dev, 1),
            lax.dynamic_slice_in_dim(conv_gate, channel_start, ff_dev, 1),
        ],
        axis=1,
    ).astype(jnp.float32)
    mixed_conv = (
        padded[:-2] * conv_taps[0] + padded[1:-1] * conv_taps[1] + padded[2:] * conv_taps[2]
    )
    hidden = (jax.nn.silu(mixed_conv[:, ff_dev:]) * mixed_conv[:, :ff_dev]).astype(jnp.bfloat16)
    down_whole = lax.all_gather(down_weight, "sp", axis=1, tiled=True)
    down_terms = jnp.dot(hidden, down_whole, preferred_element_type=jnp.float32)
    reduced = lax.psum_scatter(
        down_terms.astype(jnp.bfloat16), "tp", scatter_dimension=0, tiled=True
    ).astype(jnp.float32)
    return (stream_wide + rms_norm(widened(reduced), ffn_gain)).astype(jnp.bfloat16)


def solution(mesh):
    placed = (
        P("sp", None),
        P("sp", "tp", None),
        P("sp", "tp", None),
        P("sp", None),
        P("sp", None),
        P(),
        P(),
        P(),
        P("tp", None),
        P(),
        P(),
        P(),
        P("sp", "tp"),
        P("sp", "tp"),
        P(),
        P(),
        P("tp", "sp"),
    )
    return jax.shard_map(
        body, mesh=mesh, in_specs=placed, out_specs=P(("sp", "tp"), None), check_vma=False
    )
```

```python
import functools

import jax
import jax.numpy as jnp
from jax import lax
from jax.experimental import pallas as pl
from jax.experimental.pallas import tpu as pltpu
from jax.sharding import PartitionSpec as P

GRID = 64


epsilon = 1e-06
rope_base = 10000.0


def extended(x, sides, width):
    for axis, dim in sides:
        size, length = (lax.axis_size(axis), x.shape[dim])
        up = [(i, (i + 1) % size) for i in range(size - 1)]
        down = [(j, i) for i, j in up]
        last = lax.slice_in_dim(x, length - width, length, axis=dim)
        initial = lax.slice_in_dim(x, 0, width, axis=dim)
        before = lax.ppermute(last, axis, up)
        after = lax.ppermute(initial, axis, down)
        x = jnp.concatenate([before, x, after], axis=dim)
    return x


def rms_norm(values, gain):
    return (
        values
        * lax.rsqrt(jnp.mean(values * values, axis=-1, keepdims=True) + epsilon)
        * gain.astype(jnp.float32)
    )


def widened(values):
    return lax.optimization_barrier(values.astype(jnp.bfloat16)).astype(jnp.float32)


def rotate(values, positions):
    pair_count = values.shape[-1] // 4
    frequency = rope_base ** (-jnp.arange(pair_count, dtype=jnp.float32) / pair_count)
    grid_rows = (positions // GRID).astype(jnp.float32)
    grid_cols = (positions % GRID).astype(jnp.float32)
    angles = jnp.stack([grid_rows, grid_cols], axis=-1)[:, :, None] * frequency
    table_shape = (angles.shape[0],) + (1,) * (values.ndim - 2) + angles.shape[1:]
    cosine = jnp.cos(angles).reshape(table_shape)
    sine = jnp.sin(angles).reshape(table_shape)
    halves = values.reshape(values.shape[:-1] + (2, 2, pair_count))
    leading = halves[..., 0, :]
    trailing = halves[..., 1, :]
    turned = jnp.stack(
        [leading * cosine - trailing * sine, trailing * cosine + leading * sine], axis=-2
    )
    return turned.reshape(values.shape)


LANES = 128
CHUNKS = 4
EARLY = [0, 1]
MESH = pl.DeviceIdType.MESH


def kernel_fits(residual, latent, up_value):
    size = lax.axis_size("sp")
    return (
        size % 4 == 0
        and size >= 8
        and lax.axis_size("tp") == 2
        and residual.shape[0] == LANES
        and latent.shape[1] % LANES == 0
        and residual.shape[1] == size * LANES
        and up_value.shape[1] % LANES == 0
        and up_value.shape[1] // LANES >= size // 2
    )


def turned_rows(values, first_position):
    quarter = values.shape[0] // 4
    pair = lax.broadcasted_iota(jnp.int32, (quarter, values.shape[1]), 0).astype(jnp.float32)
    frequency = jnp.exp(pair * (-jnp.log(jnp.float32(rope_base)) / quarter))
    positions = first_position + lax.broadcasted_iota(jnp.int32, (quarter, values.shape[1]), 1)
    shift = GRID.bit_length() - 1
    places = (jnp.right_shift(positions, shift), jnp.bitwise_and(positions, GRID - 1))
    out = []
    for half, place in enumerate(places):
        angles = place.astype(jnp.float32) * frequency
        cosine, sine = jnp.cos(angles), jnp.sin(angles)
        a = values[2 * half * quarter : (2 * half + 1) * quarter]
        b = values[(2 * half + 1) * quarter : (2 * half + 2) * quarter]
        out += [a * cosine - b * sine, b * cosine + a * sine]
    return jnp.concatenate(out, axis=0)


def schedule(nz):
    order = ["a0", "s2", "s3", "w2", "w3", "v0", "v1", "a1", "c0", "v2", "a2", "c1", "v3", "a3", "c2", "c3", "p0", "u0", "u1", "u2", "u3"]
    return [(step[0], int(step[1:])) for step in order]


def row_of(gain):
    return gain[...].astype(jnp.float32).reshape(1, gain.shape[0])


def layer_kernel(
    sizes,
    residual,
    q_flat,
    q_rope,
    latent,
    rope_key,
    kv_gain,
    key_flat,
    value_flat,
    out_weight,
    post_gain,
    pre_gain,
    ffn_gain,
    conv_value,
    conv_gate,
    up_value,
    up_gate,
    down,
    out,
    lat,
    queries,
    values_local,
    keys_t,
    attended,
    out_w,
    res,
    wup,
    wdn,
    head_part,
    head_came,
    stream,
    xs,
    ups,
    edges,
    edges_came,
    parts,
    core_came,
    y_sums,
    y_came,
    z_sums,
    z_came,
    l_recv,
    l_send,
    w_recv,
    w_send,
    pair_recv,
    pair_send,
    w_loc,
    t_sem,
    x_recv,
    x_up,
    x_dn,
    x_send,
    e_sem,
    c_send,
    c_recv,
    y_send,
    y_recv,
    z_send,
    z_recv,
    ld,
):
    n_sp, heads, tile_count, score_scale = sizes
    nz, places = n_sp // 4, n_sp // 2
    tok, width = residual.shape
    half = tok // 2
    kv = latent.shape[1]
    ff_dev = up_value.shape[1]
    base = tile_count // places
    extra = 1 if tile_count % places else 0
    main, more = base * LANES, extra * LANES
    unit = main + more
    cw = width // CHUNKS
    me, c = lax.axis_index("sp"), lax.axis_index("tp")
    z, y, x = me // 4, me // 2 % 2, me % 2
    my_place = me // 2
    peer_c, peer_x, peer_y = (me, 1 - c), (me + 1 - 2 * x, c), (me + 2 - 4 * y, c)

    def dev(zz, yy):
        return (zz * 4 + yy * 2 + x, c)

    def remote(src, dst, send, recv, to):
        return pltpu.make_async_remote_copy(
            src_ref=src, dst_ref=dst, send_sem=send, recv_sem=recv, device_id=to, device_id_type=MESH
        )

    def z_order(i):
        below, above = z, nz - 1 - z
        both = jnp.minimum(below, above)
        paired = i <= 2 * both
        dist = jnp.where(paired, (i + 1) // 2, i - both)
        down_first = jnp.where(paired, i % 2 == 1, below > above)
        return jnp.where(i == 0, z, jnp.where(down_first, z - dist, z + dist))

    barrier = pltpu.get_barrier_semaphore()
    pl.semaphore_signal(barrier, inc=1, device_id=peer_c, device_id_type=MESH)
    pl.semaphore_signal(barrier, inc=1, device_id=peer_x, device_id_type=MESH)

    @pl.loop(1, places)
    def _(k):
        p = (my_place + k) % places
        pl.semaphore_signal(barrier, inc=1, device_id=(p * 2 + x, c), device_id_type=MESH)

    def local(src, dst, sem):
        return pltpu.make_async_copy(src, dst, sem)

    def first_tile(p):
        return p * tile_count // places

    def is_long(p):
        return first_tile(p + 1) - first_tile(p) > base

    def up_rows(s):
        return pl.ds(pl.multiple_of(s * tok, tok), tok)

    def pieces(p, s):
        rows = up_rows(s)

        def group(size):
            units = pl.ds(pl.multiple_of(first_tile(p) * LANES, LANES), size)
            return [
                (up_value.at[:, units], wup.at[rows, pl.ds(0, size)], 0),
                (up_gate.at[:, units], wup.at[rows, pl.ds(unit, size)], 1),
                (down.at[units, :], wdn.at[pl.ds(0, size), rows], 2),
            ]

        return [group(main), group(unit)]

    def each(p, groups, act):
        def all_of(group):
            for copy in group:
                act(copy)

        if extra:
            long = is_long(p)
            pl.when(long)(lambda: all_of(groups[1]))
            pl.when(jnp.logical_not(long))(lambda: all_of(groups[0]))
        else:
            all_of(groups[0])

    def start(copy):
        copy.start()

    def wait_recv(copy):
        copy.wait_recv()

    def wait_send(copy):
        copy.wait_send()

    own_copies = [
        [local(src, dst, w_loc.at[i]) for src, dst, i in group] for group in pieces(my_place, me)
    ]
    each(my_place, own_copies, start)
    if extra:

        @pl.when(jnp.logical_not(is_long(my_place)))
        def _():
            wup[:, main:unit] = jnp.zeros((n_sp * tok, more), jnp.bfloat16)
            wup[:, unit + main :] = jnp.zeros((n_sp * tok, more), jnp.bfloat16)
            wdn[main:, :] = jnp.zeros((more, n_sp * tok), jnp.bfloat16)

    loads = [
        local(out_weight, out_w, ld.at[0]),
        local(residual.at[pl.ds(pl.multiple_of(c * half, half), half), :], res, ld.at[1]),
    ]
    for copy in loads:
        copy.start()

    def lat_rows(s, core):
        return lat.at[pl.ds(pl.multiple_of((s * 2 + core) * half, half), half), :]

    mine = pl.ds(pl.multiple_of(c * half, half), half)
    own = latent[mine, :].astype(jnp.float32)
    normed = (
        own * lax.rsqrt(jnp.mean(own * own, axis=-1, keepdims=True) + epsilon) * row_of(kv_gain)
    )
    keys_t[...] = turned_rows(rope_key[...].astype(jnp.float32), me * tok).T
    key_turn = keys_t[mine, :]
    own_lat = pl.ds(pl.multiple_of((me * 2 + c) * half, half), half)
    lat[own_lat, 0:kv] = normed.astype(jnp.bfloat16)
    lat[own_lat, kv : kv + LANES] = jnp.concatenate(
        [key_turn, jnp.zeros((half, LANES - key_turn.shape[1]), jnp.float32)], axis=1
    ).astype(jnp.bfloat16)

    pl.semaphore_wait(barrier, places + 1)

    def lat_copy(s, to):
        return remote(lat_rows(s, c), lat_rows(s, c), l_send.at[0], l_recv.at[s], to)

    def lat_to_core(s):
        return remote(lat_rows(s, c), lat_rows(s, c), l_send.at[0], l_recv.at[n_sp], peer_c)

    def lat_all(blocks, recv):
        rows = lat.at[pl.ds(0, blocks * half), :]
        return remote(rows, rows, l_send.at[0], l_recv.at[recv], peer_c)

    for d in range(1, nz):
        lat_copy(me, dev((z + d) % nz, y)).start()
    lat_copy(me, peer_y).start()
    lat_copy(me, peer_x).start()
    lat_to_core(me).start()

    def weight_copies(p):
        return [
            [remote(src, dst, w_send.at[p, i], w_recv.at[my_place, i], (p * 2 + x, c)) for src, dst, i in group]
            for group in pieces(p, me)
        ]

    def arrivals(p):
        return [
            [remote(dst, dst, w_send.at[0, i], w_recv.at[p, i], peer_x) for _, dst, i in group]
            for group in pieces(my_place, p * 2 + x)
        ]

    def pair_copies(ups_block, down_block):
        return [
            remote(block, block, pair_send.at[i], pair_recv.at[i], peer_x)
            for i, block in enumerate((ups_block, down_block))
        ]

    def forward(p):
        for copy in pair_copies(wup.at[up_rows(p * 2 + x), :], wdn.at[:, up_rows(p * 2 + x)]):
            copy.start()

    def pass_on(i, across):
        p = (z + nz - i) % nz * 2 + (1 - y if across else y)
        each(my_place, arrivals(p), wait_recv)
        forward(p)

    @pl.loop(1, nz)
    def _(d):
        s = (z + d) % nz * 4 + y * 2 + x
        lat_copy(s, peer_c).wait_recv()
        lat_copy(s, peer_y).start()
        lat_copy(s, peer_x).start()
        lat_to_core(s).start()

    @pl.loop(1, nz)
    def _(i):
        p = (z + i) % nz * 2 + y
        each(p, weight_copies(p), start)

    @pl.loop(0, nz)
    def _(d):
        s = (z + d) % nz * 4 + (1 - y) * 2 + x
        lat_copy(s, peer_c).wait_recv()
        lat_copy(s, peer_x).start()
        lat_to_core(s).start()

    def send_across(i):
        p = (z + i) % nz * 2 + 1 - y
        each(p, weight_copies(p), start)

    for i in EARLY:
        send_across(i)

    total_heads = key_flat.shape[0] // kv
    both = jnp.concatenate([key_flat[...], value_flat[...]], axis=1)
    flat = lax.broadcasted_iota(jnp.int32, (kv, key_flat.shape[0]), 1)
    channel = lax.broadcasted_iota(jnp.int32, (kv, key_flat.shape[0]), 0) * total_heads
    q_column = lax.broadcasted_iota(jnp.int32, (tok, tok * heads), 1)
    q_row = lax.broadcasted_iota(jnp.int32, (tok, tok * heads), 0) * heads
    for h in range(heads):
        pick = jnp.where(flat == channel + (c * heads + h), 1.0, 0.0).astype(jnp.bfloat16)
        picked = jnp.dot(pick, both, preferred_element_type=jnp.float32).astype(jnp.bfloat16)
        values_local[h] = picked[:, key_flat.shape[1] :]
        pick_q = jnp.where(q_column == q_row + h, 1.0, 0.0).astype(jnp.bfloat16)
        query = jnp.dot(pick_q, q_flat[...], preferred_element_type=jnp.float32)
        queries[h, :, 0:kv] = lax.dot_general(
            query.astype(jnp.bfloat16),
            picked[:, : key_flat.shape[1]],
            (((1,), (1,)), ((), ())),
            preferred_element_type=jnp.float32,
        ).astype(jnp.bfloat16)
        turned = turned_rows(q_rope[h].astype(jnp.float32), me * tok).T
        queries[h, :, kv : kv + LANES] = jnp.concatenate(
            [turned, jnp.zeros((tok, LANES - turned.shape[1]), jnp.float32)], axis=1
        ).astype(jnp.bfloat16)

    @pl.loop(0, 2 * nz)
    def _(i):
        s = (z + i // 2) % nz * 4 + (y + i) % 2 * 2 + 1 - x
        lat_copy(s, peer_c).wait_recv()
        lat_to_core(s).start()

    each(my_place, own_copies, lambda copy: copy.wait())
    forward(my_place)

    lat_all(n_sp, n_sp).wait_recv()

    pass_on(1, False)

    @pl.loop(0, heads)
    def _(h):
        scores = lax.dot_general(
            queries[h], lat[...], (((1,), (1,)), ((), ())), preferred_element_type=jnp.float32
        )
        top = jnp.max(scores, axis=-1, keepdims=True)
        weights = jnp.exp((scores - top) * score_scale)
        totals = jnp.sum(weights, axis=-1, keepdims=True)
        mixed = jnp.dot(weights.astype(jnp.bfloat16), lat[:, 0:kv], preferred_element_type=jnp.float32)
        mixed = (mixed / totals).astype(jnp.bfloat16)
        columns = pl.ds(pl.multiple_of(h * values_local.shape[2], LANES), values_local.shape[2])
        attended[:, columns] = jnp.dot(
            mixed, values_local[h], preferred_element_type=jnp.float32
        ).astype(jnp.bfloat16)

    loads[0].wait()

    @pl.loop(0, width // 512)
    def _(n):
        columns = pl.ds(pl.multiple_of(n * 512, 512), 512)
        head_part[:, columns] = jnp.dot(
            attended[...], out_w[:, columns], preferred_element_type=jnp.float32
        ).astype(jnp.bfloat16)

    other = pl.ds(pl.multiple_of((1 - c) * half, half), half)
    swap = remote(head_part.at[other, :], head_came, t_sem.at[0], t_sem.at[1], peer_c)
    swap.start()
    loads[1].wait()
    swap.wait_recv()
    summed = head_part[mine, :].astype(jnp.float32) + head_came[...].astype(jnp.float32)
    summed = summed.astype(jnp.bfloat16).astype(jnp.float32)
    scaled = summed * lax.rsqrt(jnp.mean(summed * summed, axis=-1, keepdims=True) + epsilon)
    wide = (res[...].astype(jnp.float32) + scaled * row_of(post_gain)).astype(jnp.bfloat16)
    stream[...] = wide
    wide = wide.astype(jnp.float32)
    inputs = wide * lax.rsqrt(jnp.mean(wide * wide, axis=-1, keepdims=True) + epsilon)
    own_row = pl.ds(pl.multiple_of(my_place * tok + c * half, half), half)
    xs[own_row, :] = (inputs * row_of(pre_gain)).astype(jnp.bfloat16)

    def x_part(b, core, q):
        return xs.at[pl.ds(pl.multiple_of(b * tok + core * half, half), half), pl.ds(pl.multiple_of(q * cw, cw), cw)]

    def x_copy(b, q, send, to):
        part = x_part(b, c, q)
        return remote(part, part, send, x_recv.at[b, q], to)

    def x_to_core(b, q):
        part = x_part(b, c, q)
        return remote(part, part, x_send.at[1], x_recv.at[b, CHUNKS], peer_c)

    def x_upward(bz, q):
        return x_copy(bz * 2 + y, q, x_up.at[bz, q], dev(jnp.minimum(z + 1, nz - 1), y))

    def x_downward(bz, q):
        return x_copy(bz * 2 + y, q, x_dn.at[bz, q], dev(jnp.maximum(z - 1, 0), y))

    def x_along(bz, q, act):
        pl.when((bz <= z) & (z < nz - 1))(lambda: act(x_upward(bz, q)))
        pl.when((bz >= z) & (z > 0))(lambda: act(x_downward(bz, q)))

    def x_half(b, send, recv):
        rows = xs.at[pl.ds(pl.multiple_of(b * half, half), half), :]
        return remote(rows, rows, send, recv, peer_c)

    def x_all(blocks, i):
        rows = xs.at[pl.ds(0, blocks * half), :]
        return remote(rows, rows, x_send.at[i], x_recv.at[0, 0], peer_c)

    def x_step(i, across):
        bz = z_order(i)
        b = bz * 2 + (1 - y if across else y)
        for q in range(CHUNKS):
            if i or across:
                x_copy(b, q, x_send.at[0], peer_c).wait_recv()
            if not across:
                x_along(bz, q, start)
                x_copy(b, q, x_send.at[0], peer_y).start()
            x_to_core(b, q).start()

    def edge_copy(b):
        return remote(edges.at[b], edges_came.at[b], e_sem.at[0], e_sem.at[1], peer_x)

    def up_step(i):
        bz = z_order(i)
        for yy in range(2):
            x_half(bz * 2 + yy, x_send.at[0], x_recv.at[bz * 2 + yy, CHUNKS]).wait_recv()
        rows = pl.ds(pl.multiple_of(bz * 2 * tok, 2 * tok), 2 * tok)
        ups[rows, :] = jnp.dot(
            xs[rows, :], wup[...], preferred_element_type=jnp.float32
        ).astype(jnp.bfloat16)
        for yy in range(2):
            b = bz * 2 + yy
            first = ups[pl.ds(pl.multiple_of(b * tok, tok), 16), :].astype(jnp.float32)[0:1]
            last = ups[pl.ds(pl.multiple_of(b * tok + tok - 16, 16), 16), :].astype(jnp.float32)[15:16]
            row = lax.broadcasted_iota(jnp.int32, (8, 2 * unit), 0)
            edges[b] = jnp.where(row == 0, first, last)
            edge_copy(b).start()

    def pair_step(_):
        for copy in pair_copies(wup.at[pl.ds(0, places * tok), :], wdn.at[:, pl.ds(0, places * tok)]):
            copy.wait_recv()

    steps = {
        "w": lambda i: pass_on(i, False),
        "v": lambda i: pass_on(i, True),
        "a": lambda i: x_step(i, False),
        "c": lambda i: x_step(i, True),
        "p": pair_step,
        "s": send_across,
        "u": up_step,
    }

    for name, i in schedule(nz):
        steps[name](i)

    remote(edges, edges_came, e_sem.at[0], e_sem.at[1], peer_x).wait_recv()

    def tap_rows(conv, skip, size):
        start_column = pl.multiple_of(c * ff_dev + first_tile(my_place) * LANES + skip, LANES)
        return conv[:, pl.ds(start_column, size)].astype(jnp.float32)

    def tap_unit(conv):
        spare = jnp.where(is_long(my_place), main, 0)
        return [tap_rows(conv, 0, main)] + [tap_rows(conv, spare, more)] * extra

    taps_wide = jnp.concatenate(tap_unit(conv_value) + tap_unit(conv_gate), axis=1)
    column = lax.broadcasted_iota(jnp.int32, (1, unit), 1)
    kept = (column < main) | is_long(my_place)

    def part_of(b):
        rows = ups[pl.ds(pl.multiple_of(b * tok, tok), tok), :].astype(jnp.float32)
        before = edges_came[jnp.maximum(b - 1 + x, 0)][1:2]
        before = jnp.where(b - 1 + x >= 0, before, 0.0)
        after = edges_came[jnp.minimum(b + x, places - 1)][0:1]
        after = jnp.where(b + x <= places - 1, after, 0.0)
        row = lax.broadcasted_iota(jnp.int32, rows.shape, 0)
        previous = jnp.where(row == 0, before, pltpu.roll(rows, 1, 0))
        following = jnp.where(row == tok - 1, after, pltpu.roll(rows, tok - 1, 0))
        mixed = previous * taps_wide[0:1] + rows * taps_wide[1:2] + following * taps_wide[2:3]
        gate = mixed[:, unit:]
        hidden = gate / (1.0 + jnp.exp(-gate)) * mixed[:, :unit]
        hidden = jnp.where(kept, hidden, 0.0).astype(jnp.bfloat16)
        parts[pl.ds(pl.multiple_of(b * tok, tok), tok), :] = jnp.dot(
            hidden, wdn[...], preferred_element_type=jnp.float32
        ).astype(jnp.bfloat16)

    def part_rows(b, core):
        return pl.ds(pl.multiple_of(b * tok + core * half, half), half)

    def core_copy(b):
        return remote(parts.at[part_rows(b, 1 - c), :], core_came.at[b], c_send.at[0], c_recv.at[b], peer_c)

    def columns_of(q):
        return pl.ds(q * cw, cw)

    def core_sum(b, q):
        return parts[part_rows(b, c), columns_of(q)].astype(jnp.float32) + core_came[
            b, :, columns_of(q)
        ].astype(jnp.float32)

    def y_copy(zz, q):
        block = (zz, slice(None), columns_of(q))
        return remote(y_sums.at[block], y_came.at[block], y_send.at[0], y_recv.at[zz, q], peer_y)

    def z_copy(zz, q):
        return remote(
            z_sums.at[zz, :, columns_of(q)], z_came.at[z, :, columns_of(q)], z_send.at[0], z_recv.at[z, q], dev(zz, y)
        )

    def z_arrival(zz, q):
        block = z_came.at[zz, :, columns_of(q)]
        return remote(block, block, z_send.at[0], z_recv.at[zz, q], peer_y)

    def make(b):
        part_of(b)
        core_copy(b).start()

    make(z_order(nz - 1) * 2 + 1 - y)

    @pl.loop(0, nz)
    def _(i):
        zz = z_order(nz - 1 - i)
        last = i == nz - 1
        make(jnp.where(last, z_order(nz - 1) * 2 + y, z_order(jnp.maximum(nz - 2 - i, 0)) * 2 + 1 - y))
        b = zz * 2 + 1 - y
        core_copy(b).wait_recv()
        for q in range(CHUNKS):
            y_sums[zz, :, columns_of(q)] = core_sum(b, q).astype(jnp.bfloat16)
            y_copy(zz, q).start()

    @pl.loop(1, nz)
    def _(i):
        make(z_order(nz - 1 - i) * 2 + y)

    @pl.loop(0, nz)
    def _(i):
        zz = z_order(nz - 1 - i)
        core_copy(zz * 2 + y).wait_recv()
        for q in range(CHUNKS):
            total = core_sum(zz * 2 + y, q)
            y_copy(zz, q).wait_recv()
            z_sums[zz, :, columns_of(q)] = (total + y_came[zz, :, columns_of(q)].astype(jnp.float32)).astype(jnp.bfloat16)
            pl.when(zz != z)(lambda: z_copy(zz, q).start())

    projected = z_sums[z].astype(jnp.float32)
    for d in range(1, nz):
        zz = (z + nz - d) % nz
        for q in range(CHUNKS):
            z_arrival(zz, q).wait_recv()
        projected = projected + z_came[zz].astype(jnp.float32)
    projected = projected.astype(jnp.bfloat16).astype(jnp.float32)
    scaled = projected * lax.rsqrt(jnp.mean(projected * projected, axis=-1, keepdims=True) + epsilon)
    out[...] = (stream[...].astype(jnp.float32) + scaled * row_of(ffn_gain)).astype(jnp.bfloat16)

    lat_all(8 * nz - 1, 0).wait_send()
    swap.wait_send()
    for copy in pair_copies(wup.at[pl.ds(0, places * tok), :], wdn.at[:, pl.ds(0, places * tok)]):
        copy.wait_send()
    x_all(nz, 0).wait_send()
    x_all(places, 1).wait_send()
    remote(edges, edges_came, e_sem.at[0], e_sem.at[1], peer_x).wait_send()
    remote(core_came, core_came, c_send.at[0], c_recv.at[0], peer_c).wait_send()
    remote(y_sums, y_sums, y_send.at[0], y_recv.at[0, 0], peer_y).wait_send()
    rest = z_sums.at[pl.ds(0, nz - 1)]
    remote(rest, rest, z_send.at[0], z_recv.at[0, 0], peer_y).wait_send()

    @pl.loop(0, places)
    def _(p):
        pl.when(p != my_place)(lambda: each(p, weight_copies(p), wait_send))

    @pl.loop(0, nz)
    def _(zz):
        for q in range(CHUNKS):
            x_along(zz, q, wait_send)


def fused_layer(
    residual,
    query_nope,
    query_rope,
    latent,
    rope_key,
    kv_gain,
    key_up,
    value_up,
    out_weight,
    post_gain,
    pre_gain,
    ffn_gain,
    up_value,
    up_gate,
    conv_value,
    conv_gate,
    down_weight,
):
    n_sp = lax.axis_size("sp")
    nz, places = n_sp // 4, n_sp // 2
    tok, width = residual.shape
    half = tok // 2
    heads, kv = query_nope.shape[1], latent.shape[1]
    rope = rope_key.shape[1]
    value_width = value_up.shape[2]
    ff_dev = up_value.shape[1]
    tile_count = ff_dev // LANES
    unit = -(-tile_count // places) * LANES
    score_scale = (query_nope.shape[2] + rope) ** (-0.5)
    dma, vmem = pltpu.SemaphoreType.DMA, pltpu.VMEM
    bf16, f32 = jnp.bfloat16, jnp.float32
    scratch = [
        vmem((n_sp * tok, kv + LANES), bf16),
        vmem((heads, tok, kv + LANES), bf16),
        vmem((heads, kv, value_width), bf16),
        vmem((tok, rope), f32),
        vmem((tok, heads * value_width), bf16),
        vmem(out_weight.shape, bf16),
        vmem((half, width), bf16),
        vmem((n_sp * tok, 2 * unit), bf16),
        vmem((unit, n_sp * tok), bf16),
        vmem((tok, width), bf16),
        vmem((half, width), bf16),
        vmem((half, width), bf16),
        vmem((places * tok, width), bf16),
        vmem((places * tok, 2 * unit), bf16),
        vmem((places, 8, 2 * unit), f32),
        vmem((places, 8, 2 * unit), f32),
        vmem((places * tok, width), bf16),
        vmem((places, half, width), bf16),
        vmem((nz, half, width), bf16),
        vmem((nz, half, width), bf16),
        vmem((nz, half, width), bf16),
        vmem((nz, half, width), bf16),
        dma((n_sp + 1,)),
        dma((1,)),
        dma((places, 3)),
        dma((places, 3)),
        dma((2,)),
        dma((2,)),
        dma((3,)),
        dma((2,)),
        dma((places, CHUNKS + 1)),
        dma((nz, CHUNKS)),
        dma((nz, CHUNKS)),
        dma((2,)),
        dma((2,)),
        dma((1,)),
        dma((places,)),
        dma((1,)),
        dma((nz, CHUNKS)),
        dma((1,)),
        dma((nz, CHUNKS)),
        dma((2,)),
    ]
    whole, apart = pl.BlockSpec(memory_space=pltpu.VMEM), pl.BlockSpec(memory_space=pl.ANY)
    sizes = (n_sp, heads, tile_count, score_scale)
    return pl.pallas_call(
        functools.partial(layer_kernel, sizes),
        out_shape=jax.ShapeDtypeStruct((half, width), bf16),
        in_specs=[apart] + [whole] * 7 + [apart] + [whole] * 5 + [apart] * 3,
        out_specs=whole,
        scratch_shapes=scratch,
        compiler_params=pltpu.CompilerParams(
            collective_id=0, has_side_effects=True, vmem_limit_bytes=60 * 1024 * 1024
        ),
    )(
        residual,
        query_nope.reshape(tok * heads, -1),
        jnp.transpose(query_rope, (1, 2, 0)),
        latent,
        rope_key.T,
        kv_gain,
        key_up.reshape(-1, key_up.shape[2]),
        value_up.reshape(-1, value_width),
        out_weight,
        post_gain,
        pre_gain,
        ffn_gain,
        conv_value,
        conv_gate,
        up_value,
        up_gate,
        down_weight,
    )


def body(
    residual,
    query_nope,
    query_rope,
    latent,
    rope_key,
    kv_gain,
    key_up,
    value_up,
    out_weight,
    post_gain,
    pre_gain,
    ffn_gain,
    up_value,
    up_gate,
    conv_value,
    conv_gate,
    down_weight,
):
    if kernel_fits(residual, latent, up_value):
        return fused_layer(
            residual,
            query_nope,
            query_rope,
            latent,
            rope_key,
            kv_gain,
            key_up,
            value_up,
            out_weight,
            post_gain,
            pre_gain,
            ffn_gain,
            up_value,
            up_gate,
            conv_value,
            conv_gate,
            down_weight,
        )
    tok_rows = residual.shape[0]
    heads_dev = query_nope.shape[1]
    value_width = value_up.shape[2]
    tp_index = lax.axis_index("tp")
    positions = lax.axis_index("sp") * tok_rows + jnp.arange(tok_rows, dtype=jnp.int32)
    score_scale = (query_nope.shape[2] + query_rope.shape[2]) ** (-0.5)
    normed = rms_norm(latent.astype(jnp.float32), kv_gain).astype(jnp.bfloat16)
    key_turn = rotate(rope_key.astype(jnp.float32), positions).astype(jnp.bfloat16)
    query_turn = rotate(query_rope.astype(jnp.float32), positions).astype(jnp.bfloat16)
    key_local = lax.dynamic_slice_in_dim(key_up, tp_index * heads_dev, heads_dev, 1)
    value_local = lax.dynamic_slice_in_dim(value_up, tp_index * heads_dev, heads_dev, 1)
    latent_width = normed.shape[1]
    joined = jnp.concatenate([normed, key_turn], axis=1)
    joined = lax.all_gather(joined, "sp", axis=0, tiled=True)
    pieces = (joined[:, :latent_width], joined[:, latent_width:])
    keys_nope = jnp.einsum(
        "nc,chd->nhd", pieces[0], key_local, preferred_element_type=jnp.float32
    ).astype(jnp.bfloat16)
    values_part = jnp.einsum(
        "nc,chd->nhd", pieces[0], value_local, preferred_element_type=jnp.float32
    ).astype(jnp.bfloat16)
    row_max = jnp.full((heads_dev, tok_rows), -1e30, jnp.float32)
    scores = (
        jnp.einsum("qhd,khd->hqk", query_nope, keys_nope, preferred_element_type=jnp.float32)
        + jnp.einsum("qhd,kd->hqk", query_turn, pieces[1], preferred_element_type=jnp.float32)
    ) * score_scale
    new_max = jnp.maximum(row_max, jnp.max(scores, axis=-1))
    weights = jnp.exp(scores - new_max[:, :, None])
    totals = jnp.sum(weights, axis=-1)
    weighted = jnp.einsum(
        "hqk,khd->hqd",
        weights.astype(jnp.bfloat16),
        values_part,
        preferred_element_type=jnp.float32,
    )
    attended = (weighted / totals[:, :, None]).astype(jnp.bfloat16)
    attended = jnp.transpose(attended, (1, 0, 2)).reshape(tok_rows, heads_dev * value_width)
    row_share = tok_rows // lax.axis_size("tp")
    summed = lax.psum_scatter(
        jnp.dot(attended, out_weight, preferred_element_type=jnp.float32).astype(jnp.bfloat16),
        "tp",
        scatter_dimension=0,
        tiled=True,
    ).astype(jnp.float32)
    own_rows = lax.dynamic_slice_in_dim(residual, tp_index * row_share, row_share, 0).astype(
        jnp.float32
    )
    stream_wide = widened(own_rows + rms_norm(widened(summed), post_gain))
    own_inputs = rms_norm(stream_wide, pre_gain).astype(jnp.bfloat16)
    inputs = lax.all_gather(own_inputs, "tp", axis=0, tiled=True)
    ff_dev = up_value.shape[1]
    up_joined = jnp.concatenate([up_value, up_gate], axis=1)
    up_whole = lax.all_gather(up_joined, "sp", axis=0, tiled=True)
    up_pair = jnp.dot(inputs, up_whole, preferred_element_type=jnp.float32).astype(jnp.bfloat16)
    padded = extended(up_pair, (("sp", 0),), 1).astype(jnp.float32)
    channel_start = tp_index * ff_dev
    conv_taps = jnp.concatenate(
        [
            lax.dynamic_slice_in_dim(conv_value, channel_start, ff_dev, 1),
            lax.dynamic_slice_in_dim(conv_gate, channel_start, ff_dev, 1),
        ],
        axis=1,
    ).astype(jnp.float32)
    mixed_conv = (
        padded[:-2] * conv_taps[0] + padded[1:-1] * conv_taps[1] + padded[2:] * conv_taps[2]
    )
    hidden = (jax.nn.silu(mixed_conv[:, ff_dev:]) * mixed_conv[:, :ff_dev]).astype(jnp.bfloat16)
    down_whole = lax.all_gather(down_weight, "sp", axis=1, tiled=True)
    down_terms = jnp.dot(hidden, down_whole, preferred_element_type=jnp.float32)
    reduced = lax.psum_scatter(
        down_terms.astype(jnp.bfloat16), "tp", scatter_dimension=0, tiled=True
    ).astype(jnp.float32)
    return (stream_wide + rms_norm(widened(reduced), ffn_gain)).astype(jnp.bfloat16)


def solution(mesh):
    placed = (
        P("sp", None),
        P("sp", "tp", None),
        P("sp", "tp", None),
        P("sp", None),
        P("sp", None),
        P(),
        P(),
        P(),
        P("tp", None),
        P(),
        P(),
        P(),
        P("sp", "tp"),
        P("sp", "tp"),
        P(),
        P(),
        P("tp", "sp"),
    )
    return jax.shard_map(
        body, mesh=mesh, in_specs=placed, out_specs=P(("sp", "tp"), None), check_vma=False
    )
```
